32 devices in a mesh: sp: 16 (over z, x, core), tp: 2 (over y).
Axes of the slice: x: 2, y: 2, z: 4, core: 2. Of those that a mesh axis runs over, the one named last changes fastest.
Arguments:
- stream: bfloat16 [4096, 2048], P('sp'), may hold values from -6 to 6
- doc_ids: int32 [4096], P('sp'), may hold values from 0 to 3, never falling along the last dimension, each value on 1 to 2048 neighbouring positions
- norm_gain: float32 [2, 2048], replicated, may hold values from 0.1 to 1.9
- w_query: bfloat16 [2, 2048, 1024], P(None, None, 'tp'), may hold values from -0.125 to 0.125
- w_key: bfloat16 [2, 2048, 1024], P(None, None, 'tp'), may hold values from -0.125 to 0.125
- w_value: bfloat16 [2, 2048, 1024], P(None, None, 'tp'), may hold values from -0.125 to 0.125
- query_gain: float32 [2, 64], replicated, may hold values from 0.4 to 7
- key_gain: float32 [2, 64], replicated, may hold values from 0.4 to 7
- offset_bias: float32 [2, 16, 8, 16], P(None, 'tp'), may hold values from -4 to 4
- w_output: bfloat16 [2, 1024, 2048], replicated, may hold values from -0.1875 to 0.1875
Outputs:
- result: bfloat16 [4096, 2048], P('sp')
The draws below stay inside these ranges and needn't reach their ends.
Inputs may be any that keep to these rules, and one draw needn't show every extreme that they name: `doc_ids`: numbers never fall along the sequence; each document holds 1 to 2048 positions and one holds exactly 2048.
All inputs are finite; a program needn't handle non-finite values.
Results may differ from the reference program's by a relative error of at most 0.034.
The reference program's roundings to bfloat16 on the way (of `normed`, `queries`, `values`, `weights` and `attended`) count: a program that leaves them out, or rounds other values in their place, can miss the bound.
Values may be sent and summed in bfloat16 or wider, within the bound.
No kernel may reach another device: no remote copies, remote signals or barrier semaphores. Data moves between devices by JAX's collectives and lax.ppermute only.
A program may use at most 128 MiB of HBM per device.

```python
import math
import jax
import jax.numpy as jnp
import numpy as np
from jax import lax

D = 2048
HEADS = 16
HEAD_DIM = 64
GRID_W = 64
WIN_ROWS = 8
WIN_COLS = 16
LAYERS = 2
TOKENS = 4096
DOCS = 4
DOC_MOST = 2048


def draw_query_gain(key, part):
    fresh = jax.random.fold_in(key, 11)
    return jnp.clip(1.0 + 0.18 * jax.random.normal(fresh, (LAYERS, HEAD_DIM), jnp.float32), 0.45, 1.55)


def draw_key_gain(key, part):
    fresh = jax.random.fold_in(key, 23)
    return jnp.clip(1.0 + 0.18 * jax.random.normal(fresh, (LAYERS, HEAD_DIM), jnp.float32), 0.45, 1.55)


def block_levels(key, dims, split, smallest, high):
    loudness, own = 1.0, jax.random.fold_in(key, 6)
    for position, shards_of in split:
        heights = jnp.exp(jax.random.uniform(jax.random.fold_in(own, position), (shards_of,), jnp.float32, smallest / len(split), high / len(split)))
        loudness = loudness * jnp.repeat(heights, dims[position] // shards_of).reshape([-1 if axis == position else 1 for axis in range(len(dims))])
    return loudness


def length_profile(number_of, total, reach, slope):
    portions = [(1 << 20) // math.isqrt(rank ** slope) + 1 for rank in range(2, number_of + 1)]
    spare, given = total - reach - (number_of - 1), [1] * (number_of - 1)
    while spare > 0:
        candidates = [i for i in range(number_of - 1) if given[i] < reach]
        whole, remaining = sum([portions[i] for i in candidates]), spare
        for i in candidates:
            addition = min(reach - given[i], max(1, remaining * portions[i] // whole), spare)
            given[i] = given[i] + addition
            spare = spare - addition
    return np.array([reach] + given)


def uneven_parts(rng, count, total, bound, lean):
    if count == 2:
        one = jax.random.randint(rng, (), max(1, total - bound), min(bound, total - 1) + 1)
        return jnp.stack([one, total - one])
    tallies = jnp.asarray(length_profile(count, total, bound, lean), jnp.int32)
    twos = (count - 1) // 2
    donor, receiver = tallies[1:1 + 2 * twos:2], tallies[2:2 + 2 * twos:2]
    room = jnp.minimum(donor - 1, bound - receiver)
    passed = jax.random.randint(jax.random.fold_in(rng, 1), (twos,), 0, 1 << 20) % (room + 1)
    tallies = tallies.at[1:1 + 2 * twos:2].set(donor - passed).at[2:2 + 2 * twos:2].set(receiver + passed)
    return tallies[jax.random.permutation(jax.random.fold_in(rng, 2), count)]


def bell_draw(rng, extent, spread, bound, split=(), kind=jnp.bfloat16):
    values = spread * jax.random.normal(rng, extent, jnp.float32)
    if split:
        values = values * block_levels(rng, extent, split, -0.22, 0.18)
    return jnp.clip(values, -bound, bound).astype(kind)


def setup_inputs(seed: int = 0) -> dict:
    key_list = jax.random.split(jax.random.key(seed), 11)
    return {
        "stream": bell_draw(key_list[0], (TOKENS, D), 1.0, 6.0, ((0, 16),)),
        "doc_ids": jnp.searchsorted(jnp.cumsum(uneven_parts(key_list[1], DOCS, TOKENS, DOC_MOST, 0)), jnp.arange(TOKENS), side="right").astype(jnp.int32),
        "norm_gain": jnp.clip(1.0 + 0.18 * jax.random.normal(key_list[2], (LAYERS, D), jnp.float32), 0.1, 1.9),
        "w_query": bell_draw(key_list[3], (LAYERS, D, HEADS * HEAD_DIM), D ** -0.5, 0.125, ((2, 2),)),
        "w_key": bell_draw(key_list[4], (LAYERS, D, HEADS * HEAD_DIM), D ** -0.5, 0.125, ((2, 2),)),
        "w_value": bell_draw(key_list[5], (LAYERS, D, HEADS * HEAD_DIM), D ** -0.5, 0.125, ((2, 2),)),
        "query_gain": draw_query_gain(jax.random.fold_in(key_list[10], 71), 0),
        "key_gain": draw_key_gain(jax.random.fold_in(key_list[10], 71), 0),
        "offset_bias": bell_draw(key_list[8], (LAYERS, HEADS, WIN_ROWS, WIN_COLS), 1.0, 4.0, ((1, 2),), jnp.float32),
        "w_output": bell_draw(key_list[9], (LAYERS, HEADS * HEAD_DIM, D), (HEADS * HEAD_DIM) ** -0.5, 0.1875),
    }


eps = 1e-06

def head_norm(raw_rows, gain_row):
    split_rows = raw_rows.reshape(raw_rows.shape[0], -1, HEAD_DIM)
    inverse = lax.rsqrt(lax.optimization_barrier(jnp.mean(split_rows * split_rows, axis=-1, keepdims=True)) + eps)
    return (split_rows * inverse * gain_row).astype(jnp.bfloat16).reshape(raw_rows.shape)

def offset_table(head_bias):
    key_reach = 2 * WIN_COLS - 1
    offsets = jnp.arange(key_reach, dtype=jnp.int32)[None, :] - jnp.arange(WIN_COLS, dtype=jnp.int32)[:, None]
    inside = (offsets >= 0) & (offsets < WIN_COLS)
    one_hot = (offsets[:, :, None] == jnp.arange(WIN_COLS, dtype=jnp.int32)[None, None, :]).astype(jnp.float32)
    lookup = jnp.einsum('hjc,qkc->qhjk', head_bias, one_hot, precision=lax.Precision.HIGHEST)
    return (lookup, inside)

def window_attend(queries, pair_pad, query_marks, mark_pad, head_bias):
    heads_here = head_bias.shape[0]
    tokens_here = queries.shape[0]
    grid_rows = tokens_here // GRID_W
    col_blocks = GRID_W // WIN_COLS
    key_reach = 2 * WIN_COLS - 1
    margin = WIN_COLS // 2
    col_pad = ((0, 0), (margin, WIN_COLS - 1 - margin))
    pair_grid = jnp.pad(pair_pad.reshape(grid_rows + WIN_ROWS, GRID_W, -1), col_pad + ((0, 0),))
    mark_grid = jnp.pad(mark_pad.reshape(grid_rows + WIN_ROWS, GRID_W), col_pad)
    pair_band = jnp.stack([pair_grid[row_shift:row_shift + grid_rows] for row_shift in range(WIN_ROWS)], axis=1)
    mark_band = jnp.stack([mark_grid[row_shift:row_shift + grid_rows] for row_shift in range(WIN_ROWS)], axis=1)
    pair_win = jnp.stack([pair_band[:, :, col_block * WIN_COLS:col_block * WIN_COLS + key_reach] for col_block in range(col_blocks)], axis=2)
    mark_win = jnp.stack([mark_band[:, :, col_block * WIN_COLS:col_block * WIN_COLS + key_reach] for col_block in range(col_blocks)], axis=2)
    pair_win = pair_win.reshape(grid_rows, WIN_ROWS, col_blocks, key_reach, 2, heads_here, HEAD_DIM)
    key_win = pair_win[:, :, :, :, 0]
    value_win = pair_win[:, :, :, :, 1]
    query_grid = queries.reshape(grid_rows, col_blocks, WIN_COLS, heads_here, HEAD_DIM)
    scores = jnp.einsum('rbqhd,rjbkhd->rbqhjk', query_grid.astype(jnp.float32), key_win.astype(jnp.float32))
    lookup, inside = offset_table(head_bias)
    own_marks = query_marks.reshape(grid_rows, col_blocks, WIN_COLS)
    same_doc = mark_win.transpose(0, 2, 1, 3)[:, :, None, :, :] == own_marks[:, :, :, None, None]
    allowed = same_doc & inside[None, None, :, None, :]
    scores = scores * HEAD_DIM ** (-0.5) + lookup[None, None]
    scores = jnp.where(allowed[:, :, :, None], scores, -jnp.inf)
    highest = lax.optimization_barrier(jnp.max(scores, axis=(4, 5), keepdims=True))
    shifted_exp = jnp.exp(scores - highest)
    weights = (shifted_exp / lax.optimization_barrier(jnp.sum(shifted_exp, axis=(4, 5), keepdims=True))).astype(jnp.bfloat16)
    mixed = jnp.einsum('rbqhjk,rjbkhd->rbqhd', weights.astype(jnp.float32), value_win.astype(jnp.float32))
    return mixed.astype(jnp.bfloat16).reshape(tokens_here, heads_here * HEAD_DIM)

def reference(stream, doc_ids, norm_gain, w_query, w_key, w_value, query_gain, key_gain, offset_bias, w_output):
    hidden = stream
    marks = doc_ids + 1
    halo_tokens = WIN_ROWS // 2 * GRID_W
    mark_pad = jnp.pad(marks, (halo_tokens, halo_tokens))
    for layer_index in range(LAYERS):
        token_rows = hidden.astype(jnp.float32)
        inv_rms = lax.rsqrt(lax.optimization_barrier(jnp.mean(token_rows * token_rows, axis=-1, keepdims=True)) + eps)
        normed = (token_rows * inv_rms * norm_gain[layer_index]).astype(jnp.bfloat16)
        queries = head_norm(jnp.dot(normed, w_query[layer_index], preferred_element_type=jnp.float32), query_gain[layer_index])
        key_rows = head_norm(jnp.dot(normed, w_key[layer_index], preferred_element_type=jnp.float32), key_gain[layer_index])
        value_rows = jnp.dot(normed, w_value[layer_index], preferred_element_type=jnp.float32).astype(jnp.bfloat16)
        layer_bias = offset_bias[layer_index]

        def one_head(head_number):
            start_col = head_number * HEAD_DIM
            head_query = lax.dynamic_slice_in_dim(queries, start_col, HEAD_DIM, 1)
            head_pairs = jnp.concatenate([lax.dynamic_slice_in_dim(key_rows, start_col, HEAD_DIM, 1), lax.dynamic_slice_in_dim(value_rows, start_col, HEAD_DIM, 1)], axis=1)
            pair_pad = jnp.pad(head_pairs, ((halo_tokens, halo_tokens), (0, 0)))
            head_bias = lax.dynamic_slice_in_dim(layer_bias, head_number, 1, 0)
            return window_attend(head_query, pair_pad, marks, mark_pad, head_bias)
        per_head = lax.map(one_head, jnp.arange(HEADS, dtype=jnp.int32))
        attended = per_head.transpose(1, 0, 2).reshape(hidden.shape[0], HEADS * HEAD_DIM)
        projected = jnp.dot(attended, w_output[layer_index], preferred_element_type=jnp.float32)
        hidden = (hidden.astype(jnp.float32) + projected).astype(jnp.bfloat16)
    return hidden
```

```python
import functools

import jax
import jax.numpy as jnp
from jax import lax
from jax.experimental import pallas as pl
from jax.experimental.pallas import tpu as pltpu
from jax.sharding import PartitionSpec as P

HEAD_DIM = 64
GRID_W = 64
WIN_ROWS = 8
WIN_COLS = 16
ROWS_UP = WIN_ROWS // 2
ROWS_DOWN = WIN_ROWS - 1 - ROWS_UP
LANES = 128
MARK_ROWS = 16
WINDOW = WIN_ROWS * GRID_W
FAR = -1e30
EPS = 1e-06
VMEM_LIMIT = 28 << 20

bf16, f32 = jnp.bfloat16, jnp.float32
VMEM = pl.BlockSpec(memory_space=pltpu.VMEM)
ANY = pl.BlockSpec(memory_space=pl.ANY)
SMEM = pl.BlockSpec(memory_space=pltpu.SMEM)


def call(kernel, outs, operands, specs, scratch=(), flops=0, name=None):
    return pl.pallas_call(
        kernel,
        out_shape=outs,
        in_specs=specs,
        out_specs=jax.tree.map(lambda _: VMEM, outs),
        scratch_shapes=list(scratch),
        compiler_params=pltpu.CompilerParams(vmem_limit_bytes=VMEM_LIMIT),
        cost_estimate=pl.CostEstimate(flops=flops, bytes_accessed=1 << 20, transcendentals=0),
        name=name,
    )(*operands)


def normalise(rows, gain):
    inv_rms = lax.rsqrt(jnp.mean(rows * rows, axis=-1, keepdims=True) + EPS)
    return (rows * inv_rms * gain).astype(bf16)


def head_norm(raw, gain_row, scale=1.0):
    width = raw.shape[1]
    squares = raw * raw
    high = squares.astype(bf16)
    low = (squares - high.astype(f32)).astype(bf16)
    same = (
        lax.broadcasted_iota(jnp.int32, (width, width), 0) // HEAD_DIM
        == lax.broadcasted_iota(jnp.int32, (width, width), 1) // HEAD_DIM
    ).astype(bf16)
    sums = jnp.dot(high, same, preferred_element_type=f32) + jnp.dot(
        low, same, preferred_element_type=f32
    )
    inverse = lax.rsqrt(sums * (1.0 / HEAD_DIM) + EPS)
    gains = jnp.concatenate([gain_row] * (width // HEAD_DIM), axis=1)
    normed = (raw * inverse * gains).astype(bf16)
    return normed if scale == 1.0 else normed * jnp.asarray(scale, bf16)


def column_copies(source, layer, target, sems, first, width):
    count = target.shape[1] // width
    return [
        pltpu.make_async_copy(
            source.at[layer, :, pl.ds(i * width, width)],
            target.at[:, pl.ds(i * width, width)],
            sems.at[first + i],
        )
        for i in range(count)
    ]


def write_pairs(normed, layer, width, key_gain, wk, wv, k_copies, v_copies, marks, payloads):
    tokens = normed.shape[0]
    reach = ROWS_DOWN * GRID_W
    for g, (down, up) in enumerate(payloads):
        cols = slice(g * width, (g + 1) * width)
        k_copies[g].wait()
        raw = jnp.dot(normed, wk[:, cols], preferred_element_type=f32)
        keys = head_norm(raw, key_gain[layer : layer + 1])
        down[:tokens, :width] = keys
        up[:reach, :width] = keys[:reach]
        v_copies[g].wait()
        vals = jnp.dot(normed, wv[:, cols], preferred_element_type=f32).astype(bf16)
        down[:tokens, width:] = vals
        up[:reach, width:] = vals[:reach]
        if marks is not None and g == 0:
            rows = marks[...].astype(f32) + 1.0
            rows = jnp.concatenate(
                [rows, jnp.zeros((MARK_ROWS - rows.shape[0], LANES), f32)], axis=0
            ).astype(bf16)
            down[tokens:, :LANES] = rows
            up[reach:, :LANES] = rows
            if 2 * width > LANES:
                rest = jnp.zeros((MARK_ROWS, 2 * width - LANES), bf16)
                down[tokens:, LANES:] = rest
                up[reach:, LANES:] = rest


def enter_kernel(layer, width, groups, *refs):
    h, marks, norm_gain, key_gain, w_key, w_value = refs[:6]
    normed_out = refs[6]
    payloads = [(refs[7 + 2 * g], refs[8 + 2 * g]) for g in range(groups)]
    wk, wv, sems = refs[7 + 2 * groups :]
    k_copies = column_copies(w_key, layer, wk, sems, 0, width)
    v_copies = column_copies(w_value, layer, wv, sems, groups, width)
    for k_copy, v_copy in zip(k_copies, v_copies):
        k_copy.start()
        v_copy.start()
    normed = normalise(h[...].astype(f32), norm_gain[layer : layer + 1])
    normed_out[...] = normed
    write_pairs(normed, layer, width, key_gain, wk, wv, k_copies, v_copies, marks, payloads)


def out_project(layer, parts, w_out, wo, sems, first, h, h_out, heads_all, place):
    chunk = wo.shape[1] // 4
    copies = column_copies(w_out, layer, wo, sems, first, chunk)
    for copy in copies:
        copy.start()

    def finish():
        if place is None:
            attended = parts[0][...]
        else:
            half = heads_all.shape[1] // 2
            mine = place[0] * half
            other = half - mine
            width = parts[0].shape[1]
            for g in range(len(parts) // 2):
                heads_all[:, pl.ds(pl.multiple_of(mine + g * width, width), width)] = parts[g][...]
                heads_all[:, pl.ds(pl.multiple_of(other + g * width, width), width)] = parts[
                    len(parts) // 2 + g
                ][...]
            attended = heads_all[...]
        for i, copy in enumerate(copies):
            cols = slice(i * chunk, (i + 1) * chunk)
            copy.wait()
            update = jnp.dot(attended, wo[:, cols], preferred_element_type=f32)
            h_out[:, cols] = (h[:, cols].astype(f32) + update).astype(bf16)

    return finish


def middle_kernel(layer, width, groups, part_count, placed, *refs):
    refs = list(refs)
    place = refs.pop(0) if placed else None
    parts = refs[:part_count]
    h, norm_gain, key_gain, w_out, w_key, w_value = refs[part_count : part_count + 6]
    refs = refs[part_count + 6 :]
    h_out, normed_out = refs[:2]
    payloads = [(refs[2 + 2 * g], refs[3 + 2 * g]) for g in range(groups)]
    wo, wk, wv, heads_all, sems = refs[2 + 2 * groups :]
    finish = out_project(layer - 1, parts, w_out, wo, sems, 2 * groups, h, h_out, heads_all, place)
    k_copies = column_copies(w_key, layer, wk, sems, 0, width)
    v_copies = column_copies(w_value, layer, wv, sems, groups, width)
    for k_copy, v_copy in zip(k_copies, v_copies):
        k_copy.start()
        v_copy.start()
    finish()
    normed = normalise(h_out[...].astype(f32), norm_gain[layer : layer + 1])
    normed_out[...] = normed
    write_pairs(normed, layer, width, key_gain, wk, wv, k_copies, v_copies, None, payloads)


def leave_kernel(layer, part_count, placed, *refs):
    refs = list(refs)
    place = refs.pop(0) if placed else None
    parts = refs[:part_count]
    h, w_out, h_out, wo, heads_all, sems = refs[part_count:]
    out_project(layer, parts, w_out, wo, sems, 0, h, h_out, heads_all, place)()


def query_kernel(layer, normed, query_gain, bias, w_query, q_out, table, wq, sems):
    width = wq.shape[1]
    copies = column_copies(w_query, layer, wq, sems, 0, width)
    copies[0].start()
    heads = table.shape[0]
    span = table.shape[2]
    shape = (WIN_ROWS * WIN_COLS, span)
    source = lax.broadcasted_iota(jnp.int32, shape, 0)
    lane = lax.broadcasted_iota(jnp.int32, shape, 1)
    block, lane = lane // LANES, lane % LANES
    half = WIN_COLS // 2
    low = (lane < half) | (lane >= LANES - half)
    mid = (lane >= GRID_W - half) & (lane < GRID_W + half)
    row = 2 * block + mid.astype(jnp.int32)
    col = jnp.where(mid, lane - GRID_W + half, jnp.where(lane < half, lane + half, lane - LANES + half))
    wanted = jnp.where(low | mid, row * WIN_COLS + col, -1)
    pick = (source == wanted).astype(f32)
    base = jnp.dot(
        bias[layer], pick, preferred_element_type=f32, precision=lax.Precision.HIGHEST
    )
    tile = (GRID_W, LANES)
    offset = lax.broadcasted_iota(jnp.int32, tile, 1) % GRID_W - lax.broadcasted_iota(
        jnp.int32, tile, 0
    )
    inside = (offset >= -half) & (offset < half)
    for head in range(heads):
        for p in range(span // LANES):
            cols = slice(p * LANES, (p + 1) * LANES)
            rows = jnp.broadcast_to(base[head : head + 1, cols], tile)
            rolled = pltpu.roll(rows, 0, 1, stride=1, stride_axis=0)
            table[head, :, cols] = jnp.where(inside, rolled, FAR)
    copies[0].wait()
    raw = jnp.dot(normed[...], wq[...], preferred_element_type=f32)
    q_out[...] = head_norm(raw, query_gain[layer : layer + 1], HEAD_DIM ** (-0.5))


def mark_line(payload, start, tokens):
    return [payload[start + i : start + i + 1, :LANES].astype(f32) for i in range(tokens // LANES)]


def write_mask(own, low, high, tokens, mask):
    reach = ROWS_DOWN * GRID_W
    line = mark_line(low, tokens, tokens) + mark_line(own, tokens, tokens)
    line = jnp.concatenate(line + mark_line(high, reach, tokens), axis=1)
    total = line.shape[1]
    line = jnp.broadcast_to(line, (8, total))
    own_rows = [
        jnp.broadcast_to(one, (LANES, LANES)).T for one in mark_line(own, tokens, tokens)
    ]
    own_rows = jnp.concatenate(own_rows, axis=0)
    for r in range(tokens // GRID_W):
        shifted = line if r == 0 else pltpu.roll(line, total - r * GRID_W, 1)
        mine = own_rows[r * GRID_W : (r + 1) * GRID_W]
        mine = jnp.concatenate([mine] * (WINDOW // LANES), axis=1)
        mask[r * GRID_W : (r + 1) * GRID_W] = jnp.where(mine == shifted[:1, :WINDOW], 0.0, FAR)


def attend_kernel(group, width, tokens, make_mask, *refs):
    q, table, own, low, high = refs[:5]
    if make_mask:
        out, mask = refs[5:]
        write_mask(own, low, high, tokens, mask)
    else:
        mask, out = refs[5:]
    step = min(LANES, width)
    heads = step // HEAD_DIM
    first = group * width
    ones = jnp.ones((WINDOW, step), bf16)
    for p in range(width // step):
        lanes = slice(p * step, (p + 1) * step)
        v_lanes = slice(width + p * step, width + (p + 1) * step)
        head0 = (first + p * step) // HEAD_DIM
        for r in range(tokens // GRID_W):
            mine = slice(r * GRID_W, (r + 1) * GRID_W)
            rows = q[mine, first + p * step : first + (p + 1) * step]
            pieces = [low[r * GRID_W : tokens, lanes], own[:tokens, lanes]]
            v_pieces = [low[r * GRID_W : tokens, v_lanes], own[:tokens, v_lanes]]
            if r:
                pieces.append(high[: r * GRID_W, lanes])
                v_pieces.append(high[: r * GRID_W, v_lanes])
            keys = jnp.concatenate(pieces, axis=0)
            vals = jnp.concatenate(v_pieces, axis=0)
            if heads > 1:
                lane = lax.broadcasted_iota(jnp.int32, rows.shape, 1) // HEAD_DIM
                rows = jnp.concatenate(
                    [jnp.where(lane == i, rows, jnp.zeros_like(rows)) for i in range(heads)], axis=0
                )
            scores = lax.dot_general(
                rows, keys, (((1,), (1,)), ((), ())), preferred_element_type=f32
            )
            near = mask[mine]
            scores = scores + jnp.concatenate(
                [table[head0 + i] + near for i in range(heads)], axis=0
            )
            top = jnp.max(scores, axis=1, keepdims=True)
            weights = jnp.exp(scores - top).astype(bf16)
            mixed = jnp.dot(
                weights, jnp.concatenate([vals, ones], axis=1), preferred_element_type=f32
            )
            mixed = mixed[:, :step] / mixed[:, step:]
            if heads > 1:
                lane = lax.broadcasted_iota(jnp.int32, (GRID_W, step), 1) // HEAD_DIM
                result = mixed[:GRID_W]
                for i in range(1, heads):
                    result = jnp.where(lane == i, mixed[i * GRID_W : (i + 1) * GRID_W], result)
                mixed = result
            out[mine, lanes] = mixed.astype(bf16)


def on_device(
    stream, doc_ids, norm_gain, w_query, w_key, w_value, query_gain, key_gain, offset_bias, w_output
):
    tokens, model = stream.shape
    layers, _, local = w_query.shape
    heads = local // HEAD_DIM
    every = w_output.shape[1]
    groups = 2 if local % (4 * HEAD_DIM) == 0 else 1
    width = local // groups
    reach = ROWS_DOWN * GRID_W
    ranks = lax.axis_size("sp")
    tensor = lax.axis_size("tp")
    swap = tensor == 2
    forward = [(i, i + 1) for i in range(ranks - 1)]
    backward = [(i + 1, i) for i in range(ranks - 1)]
    marks = doc_ids.reshape(tokens // LANES, LANES)
    bias = offset_bias.reshape(layers, heads, WIN_ROWS * WIN_COLS)
    place = [lax.axis_index("tp").astype(jnp.int32).reshape(1)] if swap else []
    weight = pltpu.VMEM((model, local), bf16)

    def payload_shapes(marked):
        shapes = []
        for g in range(groups):
            extra = MARK_ROWS if marked and g == 0 else 0
            shapes.append(jax.ShapeDtypeStruct((tokens + extra, 2 * width), bf16))
            shapes.append(jax.ShapeDtypeStruct((reach + extra, 2 * width), bf16))
        return shapes

    rows_shape = jax.ShapeDtypeStruct((tokens, model), bf16)
    pair_flops = 4 * tokens * model * local
    out_flops = 2 * tokens * every * model
    normed, *payloads = call(
        functools.partial(enter_kernel, 0, width, groups),
        [rows_shape] + payload_shapes(True),
        (stream, marks, norm_gain, key_gain, w_key, w_value),
        [VMEM] * 4 + [ANY] * 2,
        [weight, weight, pltpu.SemaphoreType.DMA((2 * groups,))],
        flops=pair_flops,
        name="enter",
    )
    current = stream
    mask = None
    for layer in range(layers):
        arrived = []
        for g in range(groups):
            down, up = payloads[2 * g], payloads[2 * g + 1]
            arrived.append(
                (down, lax.ppermute(down, "sp", forward), lax.ppermute(up, "sp", backward))
            )
        queries, table = call(
            functools.partial(query_kernel, layer),
            [
                jax.ShapeDtypeStruct((tokens, local), bf16),
                jax.ShapeDtypeStruct((heads, GRID_W, WINDOW), f32),
            ],
            (normed, query_gain, bias, w_query),
            [VMEM] * 3 + [ANY],
            [weight, pltpu.SemaphoreType.DMA((1,))],
            flops=pair_flops // 2,
            name="query",
        )
        attended = []
        for g in range(groups):
            make_mask = mask is None
            outs = [jax.ShapeDtypeStruct((tokens, width), bf16)]
            operands = [queries, table, *arrived[g]]
            if make_mask:
                outs.append(jax.ShapeDtypeStruct((tokens, WINDOW), f32))
            else:
                operands.append(mask)
            results = call(
                functools.partial(attend_kernel, g, width, tokens, make_mask),
                outs,
                operands,
                [VMEM] * len(operands),
                flops=4 * tokens * WINDOW * 2 * width,
                name="attend",
            )
            attended.append(results[0])
            if make_mask:
                mask = results[1]
        if swap:
            pairs = [(0, 1), (1, 0)]
            parts = attended + [lax.ppermute(part, "tp", pairs) for part in attended]
        else:
            own = attended[0] if groups == 1 else jnp.concatenate(attended, axis=1)
            parts = [lax.all_gather(own, "tp", axis=1, tiled=True)]
        whole_out = pltpu.VMEM((every, model), bf16)
        heads_all = pltpu.VMEM((tokens, every), bf16)
        if layer + 1 < layers:
            current, normed, *payloads = call(
                functools.partial(middle_kernel, layer + 1, width, groups, len(parts), swap),
                [rows_shape, rows_shape] + payload_shapes(False),
                (*place, *parts, current, norm_gain, key_gain, w_output, w_key, w_value),
                [SMEM] * len(place) + [VMEM] * (len(parts) + 3) + [ANY] * 3,
                [whole_out, weight, weight, heads_all, pltpu.SemaphoreType.DMA((2 * groups + 4,))],
                flops=pair_flops + out_flops,
                name="middle",
            )
        else:
            (current,) = call(
                functools.partial(leave_kernel, layer, len(parts), swap),
                [rows_shape],
                (*place, *parts, current, w_output),
                [SMEM] * len(place) + [VMEM] * (len(parts) + 1) + [ANY],
                [whole_out, heads_all, pltpu.SemaphoreType.DMA((4,))],
                flops=out_flops,
                name="leave",
            )
    return current


def solution(mesh):
    return jax.shard_map(
        on_device,
        mesh=mesh,
        in_specs=(
            P("sp", None),
            P("sp"),
            P(),
            P(None, None, "tp"),
            P(None, None, "tp"),
            P(None, None, "tp"),
            P(),
            P(),
            P(None, "tp", None, None),
            P(),
        ),
        out_specs=P("sp", None),
        check_vma=False,
    )
```
